32 devices in a mesh: ep: 8 (over z, y), tp: 4 (over x, core).
Axes of the slice: x: 2, y: 2, z: 4, core: 2. Of those that a mesh axis runs over, the one named last changes fastest.
Arguments:
- tokens: bfloat16 [2048, 2048], P('ep'), may hold values from -6 to 6
- cotangent: bfloat16 [2048, 2048], P('ep'), may hold values from -6 to 6
- gate_weights: bfloat16 [2048, 2], P('ep'), may hold values from 0.099609375 to 0.8984375
- routes: int32 [2048, 2], P('ep'), may hold values from 0 to 7, all different within a row; in each aligned block of 256 rows (0 to 255, 256 to 511, ...) at most 96 rows name the same one
- w_gate: bfloat16 [8, 2048, 3584], P('ep', None, 'tp'), may hold values from -0.125 to 0.125
- w_up: bfloat16 [8, 2048, 3584], P('ep', None, 'tp'), may hold values from -0.125 to 0.125
- w_down: bfloat16 [8, 3584, 2048], P('ep', 'tp'), may hold values from -0.09375 to 0.09375
Outputs:
- grad_tokens: bfloat16 [2048, 2048], P('ep', 'tp')
- grad_gates: float32 [2048, 2], P('ep')
- grad_w_gate: bfloat16 [8, 2048, 3584], P('ep', None, 'tp')
- grad_w_up: bfloat16 [8, 2048, 3584], P('ep', None, 'tp')
- grad_w_down: bfloat16 [8, 3584, 2048], P('ep', 'tp')
The draws below stay inside these ranges and needn't reach their ends.
Inputs may be any that keep to these rules, and one draw needn't show every extreme that they name: `routes`: each row names 2 different experts. Among the rows of one index of ep no expert is named by more than 96 rows, and this bound is reached in every draw.
All inputs are finite; a program needn't handle non-finite values.
Results may differ from the reference program's by a relative error of at most 0.012.
Values may be sent and summed in bfloat16 or wider, within the bound.
A program may use at most 128 MiB of HBM per device.

```python
import math
import jax
import jax.numpy as jnp
import numpy as np
from jax import lax

D = 2048
FFE = 3584
TOPK = 2
TOK_DEV = 256
EXPERTS = 8
CAP = 96
TOKENS = 2048
N_EP = 8
N_TP = 4


def levels(key, extent, cuts, low, top_value):
    loudness, own = 1.0, jax.random.fold_in(key, 6)
    for position, shards_of in cuts:
        steps = jnp.exp(jax.random.uniform(jax.random.fold_in(own, position), (shards_of,), jnp.float32, low / len(cuts), top_value / len(cuts)))
        loudness = loudness * jnp.repeat(steps, extent[position] // shards_of).reshape([-1 if axis == position else 1 for axis in range(len(extent))])
    return loudness


def routed_block(own_key, own, number, rows, number_of, top, most, lean):
    order = jax.random.permutation(own_key, number_of)
    crowded, common = load_shares(number_of, rows * top, most, lean, True), load_shares(number_of, rows * top, most, lean, False)
    places = jnp.arange(number_of)

    def named(lengths, rotation):
        used = int((lengths > 0).sum())
        fixed = max(1, used // 4)
        passed = fixed + (places - fixed + rotation * (used - fixed)) % max(1, number_of - fixed)
        return jnp.zeros((number_of,), jnp.int32).at[order[jnp.where(places < fixed, places, passed)]].set(jnp.asarray(lengths, jnp.int32))

    lengths = jnp.where(number % 4 == 0, named(crowded, number // 4), named(common, number - number // 4 - 1))
    mixed = jax.random.permutation(jax.random.fold_in(own, 3), number_of)
    giver, receiver = mixed[0:number_of // 2 * 2:2], mixed[1:number_of // 2 * 2:2]
    room = jnp.minimum(lengths[giver] - 1, most - lengths[receiver]) // 2
    room = jnp.where((giver == order[0]) | (receiver == order[0]) | (lengths[receiver] == 0), 0, jnp.maximum(room, 0))
    passed = jax.random.randint(jax.random.fold_in(own, 4), (number_of // 2,), 0, 1 << 20) % (room + 1)
    lengths = lengths.at[giver].add(-passed).at[receiver].add(passed)
    items = jnp.searchsorted(jnp.cumsum(lengths), jnp.arange(rows * top), side="right").astype(jnp.int32)
    grid = items.reshape(top, rows).T
    grid = grid[jax.random.permutation(jax.random.fold_in(own, 1), rows)]
    rotation = jax.random.randint(jax.random.fold_in(own, 2), (rows, 1), 0, top)
    return jnp.take_along_axis(grid, (jnp.arange(top)[None, :] + rotation) % top, axis=1)


def load_shares(number_of, total, bound, slope, full):
    weights = [(1 << 20) // math.isqrt(grade ** slope) + 1 for grade in range(1, number_of + 1)]
    largest = bound if full else min(bound, max(-(-total // number_of), total * weights[0] // sum(weights)))
    least = 1 if total - largest >= number_of - 1 else 0
    holding, surplus = [largest] + [least] * (number_of - 1), total - largest - least * (number_of - 1)
    while surplus > 0:
        free = [i for i in range(1, number_of) if holding[i] < largest] or [i for i in range(1, number_of) if holding[i] < bound]
        pool, left = sum([weights[i] for i in free]), surplus
        for i in free:
            addition = min(bound - holding[i], max(1, left * weights[i] // pool), surplus)
            holding[i] = holding[i] + addition
            surplus = surplus - addition
    return np.array(holding)


def scatter_about(stream_key, extent, deviation, limit, cuts=(), kind=jnp.bfloat16):
    result = deviation * jax.random.normal(stream_key, extent, jnp.float32)
    if cuts:
        result = result * levels(stream_key, extent, cuts, -0.22, 0.18)
    return jnp.clip(result, -limit, limit).astype(kind)


def setup_inputs(seed: int = 0) -> dict:
    streams_of = jax.random.split(jax.random.key(seed), 8)
    tokens = scatter_about(streams_of[0], (TOKENS, D), 1.0, 6.0, ((0, 8),))
    cotangent = scatter_about(streams_of[1], (TOKENS, D), 1.0, 6.0, ((0, 8),))
    gate_weights = jnp.clip(0.099609375 + 0.7988281 * jax.random.uniform(streams_of[2], (TOKENS, TOPK), jnp.float32) ** levels(streams_of[2], (TOKENS, TOPK), ((0, 8),), -0.2, 0.2), 0.099609375, 0.8984375).astype(jnp.bfloat16)
    routes_keys = jax.random.split(jax.random.fold_in(streams_of[3], 1), TOKENS // TOK_DEV)
    routes_turns = jax.random.permutation(jax.random.fold_in(streams_of[3], 3), TOKENS // TOK_DEV)
    routes = jax.vmap(lambda own, number: routed_block(jax.random.fold_in(streams_of[3], 2), own, number, TOK_DEV, EXPERTS, TOPK, CAP, 2))(routes_keys, routes_turns).reshape((TOKENS, TOPK))
    w_gate = scatter_about(streams_of[4], (EXPERTS, D, FFE), D ** -0.5, 0.125, ((0, 8), (2, 4)))
    w_up = scatter_about(streams_of[5], (EXPERTS, D, FFE), D ** -0.5, 0.125, ((0, 8), (2, 4)))
    w_down = scatter_about(streams_of[6], (EXPERTS, FFE, D), FFE ** -0.5, 0.09375, ((0, 8), (1, 4)))
    return dict(tokens=tokens, cotangent=cotangent, gate_weights=gate_weights, routes=routes, w_gate=w_gate, w_up=w_up, w_down=w_down)


def reference(tokens, cotangent, gate_weights, routes, w_gate, w_up, w_down):
    pair_count = TOK_DEV * TOPK
    total = TOKENS * TOPK
    routed = routes.reshape(N_EP, pair_count)
    onehot = (routed[:, :, None] == jnp.arange(EXPERTS, dtype=jnp.int32)[None, None, :]).astype(jnp.int32)
    earlier = jnp.sum((jnp.cumsum(onehot, axis=1) - onehot) * onehot, axis=2)
    source = jnp.arange(N_EP, dtype=jnp.int32)[:, None]
    slot_of = routed * (N_EP * CAP) + source * CAP + earlier
    pair_of = source * pair_count + jnp.arange(pair_count, dtype=jnp.int32)[None, :]
    slot_pair = jnp.full((EXPERTS * N_EP * CAP,), total, jnp.int32)
    slot_pair = slot_pair.at[slot_of.reshape(-1)].set(pair_of.reshape(-1)).reshape(EXPERTS, N_EP * CAP)
    tok_pad = jnp.concatenate([tokens, jnp.zeros((1, D), jnp.bfloat16)], axis=0)
    cot_pad = jnp.concatenate([cotangent, jnp.zeros((1, D), jnp.bfloat16)], axis=0)
    gate_pad = jnp.concatenate([gate_weights.reshape(-1), jnp.zeros((1,), jnp.bfloat16)], axis=0)
    block_width = FFE // N_TP

    def expert_grads(packed):
        pair_ids, weight_gate, weight_up, weight_down = packed
        token_ids = jnp.where(pair_ids < total, pair_ids // TOPK, TOKENS).astype(jnp.int32)
        x_rows = tok_pad[token_ids]
        c_rows = cot_pad[token_ids]
        weights = gate_pad[pair_ids].astype(jnp.float32)
        gate_pre = jnp.dot(x_rows, weight_gate, preferred_element_type=jnp.float32)
        up_pre = jnp.dot(x_rows, weight_up, preferred_element_type=jnp.float32)
        logistic = jax.nn.sigmoid(gate_pre)
        activated = gate_pre * logistic
        hidden = (activated * up_pre).astype(jnp.bfloat16)
        back_hidden = jnp.dot(c_rows, weight_down.T, preferred_element_type=jnp.float32)
        pair_gate = jnp.sum(hidden.astype(jnp.float32) * back_hidden, axis=1)
        scaled = (weights[:, None] * c_rows.astype(jnp.float32)).astype(jnp.bfloat16)
        grad_down = jnp.dot(hidden.T, scaled, preferred_element_type=jnp.float32).astype(jnp.bfloat16)
        grad_hidden = weights[:, None] * back_hidden
        gate_grad = (grad_hidden * up_pre * logistic * (1.0 + gate_pre * (1.0 - logistic))).astype(jnp.bfloat16)
        up_grad = (grad_hidden * activated).astype(jnp.bfloat16)
        grad_gate_w = jnp.dot(x_rows.T, gate_grad, preferred_element_type=jnp.float32).astype(jnp.bfloat16)
        grad_up_w = jnp.dot(x_rows.T, up_grad, preferred_element_type=jnp.float32).astype(jnp.bfloat16)
        summed = jnp.zeros((x_rows.shape[0], D), jnp.float32)
        for block in range(N_TP):
            lower = block * block_width
            upper = lower + block_width
            part = jnp.dot(gate_grad[:, lower:upper], weight_gate[:, lower:upper].T, preferred_element_type=jnp.float32)
            part = part + jnp.dot(up_grad[:, lower:upper], weight_up[:, lower:upper].T, preferred_element_type=jnp.float32)
            summed = summed + part.astype(jnp.bfloat16).astype(jnp.float32)
        return grad_gate_w, grad_up_w, grad_down, summed.astype(jnp.bfloat16), pair_gate

    grad_w_gate, grad_w_up, grad_w_down, pair_rows, pair_gates = lax.map(
        expert_grads, (slot_pair, w_gate, w_up, w_down))
    flat_ids = slot_pair.reshape(-1)
    pair_grad = jnp.zeros((total, D), jnp.bfloat16).at[flat_ids].set(pair_rows.reshape(-1, D), mode="drop")
    grad_tokens = jnp.sum(pair_grad.reshape(TOKENS, TOPK, D).astype(jnp.float32), axis=1).astype(jnp.bfloat16)
    grad_gates = jnp.zeros((total,), jnp.float32).at[flat_ids].set(pair_gates.reshape(-1), mode="drop")
    return grad_tokens, grad_gates.reshape(TOKENS, TOPK), grad_w_gate, grad_w_up, grad_w_down
```

```python
import functools

import jax
import jax.numpy as jnp
from jax import lax
from jax.experimental import pallas as pl
from jax.experimental.pallas import tpu as pltpu
from jax.sharding import PartitionSpec as P

MESH = pl.DeviceIdType.MESH
FIRST = (((0,), (0,)), ((), ()))
SUM_ROWS = 8
STAGES = 4
NEAR = 2


def expert_kernel(groups, slot, quarter,
                  routes, weights, tokens, cotangent, w_gate, w_up, w_down,
                  og, ou, od, back_rows, back_gate, places,
                  tok, cot, sent_x, sent_c, more_x, more_c, x_rows, c_rows, wg, wu, wd, wg_t, wu_t, wd_t,
                  gate_pre, up_pre, back, hidden, grads,
                  part, core_got, x_got, total, gate_all, gate_sum,
                  load_sem, first_send, first_recv, core_send, core_recv,
                  x_send, x_recv, second_send, second_recv,
                  pair_send, pair_recv, cross_send, cross_recv, home_send, home_recv,
                  sum_send, sum_recv, sumhome_send, sumhome_recv, near_sem):
    me = lax.axis_index("ep")
    t = lax.axis_index("tp")
    core = lax.rem(t, 2)
    side = t // 2
    core_peer = side * 2 + (1 - core)
    x_peer = (1 - side) * 2 + core
    x_core_peer = (1 - side) * 2 + (1 - core)
    rows = groups * slot
    ffe = wg.shape[1]
    width = wg.shape[0]
    tok_dev = tok.shape[0]
    bf, f32 = jnp.bfloat16, jnp.float32
    bits = groups.bit_length() - 1
    stages = min(STAGES, groups)
    per = groups // stages
    span = per * slot

    def flip(j):
        out = 0
        for b in range(bits):
            s = 1 << b
            out = out + s * lax.rem(lax.rem(me // s, 2) + lax.rem(j // s, 2), 2)
        return out

    def loop(lo, hi, body):
        def step(d, c):
            body(d)
            return c
        lax.fori_loop(lo, hi, step, 0)

    barrier = pltpu.get_barrier_semaphore()

    def greet(d):
        pl.semaphore_signal(barrier, inc=1, device_id=(lax.rem(me + d, groups), t),
                            device_id_type=MESH)

    loop(1, groups, greet)
    for o in range(1, 4):
        pl.semaphore_signal(barrier, inc=1, device_id=(me, lax.rem(t + o, 4)),
                            device_id_type=MESH)
    loads = [
        pltpu.make_async_copy(src, dst, load_sem.at[i])
        for i, (src, dst) in enumerate(((tokens, tok), (cotangent, cot), (w_down, wd),
                                        (w_gate, wg), (w_up, wu)))
    ]
    for load in loads:
        load.start()

    def rblk(ref, s, size=slot):
        return ref.at[pl.ds(pl.multiple_of(s * size, size if size < 16 else 16), size)]

    def cols(q):
        return pl.ds(pl.multiple_of(q * quarter, 128), quarter)

    def blk(ref, s, q):
        return ref.at[pl.ds(pl.multiple_of(s * slot, 16), slot), cols(q)]

    def rc(src, dst, ssem, rsem, ep, tp):
        return pltpu.make_async_remote_copy(
            src_ref=src, dst_ref=dst, send_sem=ssem, recv_sem=rsem,
            device_id=(ep, tp), device_id_type=MESH)

    sent = (sent_x, sent_c)
    more = (more_x, more_c)
    full = (x_rows, c_rows)

    def first(a, j):
        return rc(rblk(sent[a], j), blk(full[a], j, t), first_send.at[a, j],
                  first_recv.at[a, j], flip(j), t)

    def to_core(a, j, q):
        return rc(blk(full[a], j, q), blk(full[a], j, q), core_send.at[a, j],
                  core_recv.at[a, j], me, core_peer)

    def to_x(a, j, q):
        return rc(blk(full[a], j, q), blk(full[a], j, q), x_send.at[a, j],
                  x_recv.at[a, j], me, x_peer)

    def direct(a, j):
        return rc(rblk(more[a], j), blk(full[a], j, x_peer), x_send.at[a, j],
                  x_recv.at[a, j], flip(j), t)

    def to_core_again(a, j, q):
        return rc(blk(full[a], j, q), blk(full[a], j, q), second_send.at[a, j],
                  second_recv.at[a, j], me, core_peer)

    kinds = lax.broadcasted_iota(jnp.int32, (groups, tok_dev), 0)
    expert = jnp.bitwise_xor(kinds, me)
    hot = [(expert == routes[k:k + 1, :]).astype(f32) for k in range(2)]
    before = (lax.broadcasted_iota(jnp.int32, (tok_dev, tok_dev), 0)
              < lax.broadcasted_iota(jnp.int32, (tok_dev, tok_dev), 1)).astype(f32).astype(bf)
    earlier = jnp.dot(jnp.concatenate(hot, axis=0).astype(bf), before, preferred_element_type=f32)
    base = (kinds * slot).astype(f32)
    counts = (base + earlier[0:groups],
              base + earlier[groups:2 * groups] + jnp.sum(hot[0], axis=1, keepdims=True))
    place = [jnp.sum(hot[k] * counts[k], axis=0, keepdims=True).astype(jnp.int32)
             for k in range(2)]
    places[...] = jnp.concatenate(
        place + [jnp.full((6, tok_dev), -1, jnp.int32)], axis=0)
    share = [weights[k:k + 1, :].astype(f32) for k in range(2)]

    def picks(j):
        at = lax.broadcasted_iota(jnp.int32, (slot, tok_dev), 0) + j * slot
        hit = [at == places[k:k + 1, :] for k in range(2)]
        plain = jnp.where(hit[0] | hit[1], 1.0, 0.0).astype(bf)
        scaled = (jnp.where(hit[0], share[0], 0.0) + jnp.where(hit[1], share[1], 0.0)).astype(bf)
        return plain, scaled

    pl.semaphore_wait(barrier, groups + 2)
    loads[0].wait()
    loads[1].wait()

    def dispatch(j):
        plain, scaled = picks(j)
        r = pl.ds(pl.multiple_of(j * slot, 16), slot)
        sent_x[r, :] = jnp.dot(plain, tok[:, cols(t)], preferred_element_type=f32).astype(bf)
        first(0, j).start()
        sent_c[r, :] = jnp.dot(scaled, cot[:, cols(t)], preferred_element_type=f32).astype(bf)
        first(1, j).start()

    def dispatch_more(j):
        plain, scaled = picks(j)
        r = pl.ds(pl.multiple_of(j * slot, 16), slot)
        more_x[r, :] = jnp.dot(plain, tok[:, cols(x_peer)], preferred_element_type=f32).astype(bf)
        direct(0, j).start()
        more_c[r, :] = jnp.dot(scaled, cot[:, cols(x_peer)], preferred_element_type=f32).astype(bf)
        direct(1, j).start()

    near = min(NEAR, groups)
    loop(1, min(2 * per, groups), dispatch)
    loop(1, near, dispatch_more)
    loop(min(2 * per, groups), groups, dispatch)
    plain, scaled = picks(0)
    x_rows[0:slot, :] = jnp.dot(plain, tok[...], preferred_element_type=f32).astype(bf)
    c_rows[0:slot, :] = jnp.dot(scaled, cot[...], preferred_element_type=f32).astype(bf)

    def blocks(g):
        return max(1, g * per), (g + 1) * per

    def arrive(a, j):
        first(a, j).wait_recv()
        to_x(a, j, t).start()
        to_core(a, j, t).start()

    def arrive_near(a, j):
        first(a, j).wait_recv()
        to_core(a, j, t).start()

    def relay(a, j):
        to_x(a, j, x_peer).wait_recv()
        to_core_again(a, j, x_peer).start()

    def settled(a, j):
        to_core(a, j, core_peer).wait_recv()
        to_core_again(a, j, x_core_peer).wait_recv()

    def each(k, fn):
        lo, hi = max(1, k * per // 2), (k + 1) * per // 2

        def run(lo, hi, fn):
            def body(j):
                fn(0, j)
                fn(1, j)
            if hi > lo:
                loop(lo, hi, body)
        if fn is arrive:
            run(lo, min(hi, near), arrive_near)
            lo = max(lo, near)
        run(lo, hi, fn)

    def turn(src, dst):
        for lo in range(0, src.shape[0], 128):
            n = min(128, src.shape[0] - lo)
            dst[:, lo:lo + n] = src[lo:lo + n, :].T

    def forward(g):
        r = slice(g * span, (g + 1) * span)
        gate_pre[...] = jnp.dot(x_rows[r, :], wg[...], preferred_element_type=f32)
        up_pre[...] = jnp.dot(x_rows[r, :], wu[...], preferred_element_type=f32)

    def backward(g):
        r = slice(g * span, (g + 1) * span)
        back[...] = jnp.dot(c_rows[r, :], wd_t[...], preferred_element_type=f32)

    lanes = gate_all.shape[2]

    def elementwise(g):
        def body(i):
            r = pl.ds(pl.multiple_of(i * slot, 16), slot)
            w = pl.ds(pl.multiple_of((g * per + i) * slot, 16), slot)
            summed = jnp.zeros((slot, 128), f32)
            for lo in range(0, ffe, 128):
                v = gate_pre[r, lo:lo + 128]
                u = up_pre[r, lo:lo + 128]
                b = back[r, lo:lo + 128]
                logistic = jax.nn.sigmoid(v)
                act = v * logistic
                h = (act * u).astype(bf)
                hidden[w, lo:lo + 128] = h
                summed = summed + h.astype(f32) * b
                grads[w, lo:lo + 128] = (b * u * logistic * (1.0 + v * (1.0 - logistic))).astype(bf)
                grads[w, ffe + lo:ffe + lo + 128] = (b * act).astype(bf)
            if lanes > slot:
                summed = jnp.concatenate([summed, jnp.zeros((lanes - slot, 128), f32)], axis=0)
            row = jnp.sum(summed.T, axis=0, keepdims=True)
            s = pl.ds(pl.multiple_of((g * per + i) * SUM_ROWS, SUM_ROWS), SUM_ROWS)
            gate_all[t, s, :] = jnp.broadcast_to(row, (SUM_ROWS, lanes))
        loop(0, per, body)

    def row_product(g, q, i):
        r = slice(g * span, (g + 1) * span)
        value = jnp.dot(grads[r, 0:ffe], wg_t[:, cols(q)], preferred_element_type=f32)
        value = value + jnp.dot(grads[r, ffe:2 * ffe], wu_t[:, cols(q)],
                                preferred_element_type=f32)
        part[i, r, :] = value.astype(bf)

    def pair(g, i):
        r = pl.ds(g * span, span)
        return rc(part.at[i, r], core_got.at[i, r], pair_send.at[i, g], pair_recv.at[i, g],
                  me, core_peer)

    def cross(s):
        return rc(rblk(part.at[2], s), rblk(x_got, s), cross_send.at[s], cross_recv.at[s],
                  me, x_peer)

    def home(j):
        return rc(rblk(total, j), rblk(back_rows, j), home_send.at[j], home_recv.at[j],
                  flip(j), t)

    def give_back(g):
        row_product(g, x_core_peer, 0)
        pair(g, 0).start()
        row_product(g, x_peer, 2)
        pair(g, 0).wait_recv()

        def add_cross(s):
            r = pl.ds(pl.multiple_of(s * slot, 16), slot)
            part[2, r, :] = (part[2, r, :].astype(f32) + core_got[0, r, :].astype(f32)).astype(bf)
            cross(s).start()
        loop(g * per, (g + 1) * per, add_cross)
        row_product(g, core_peer, 1)
        pair(g, 1).start()
        row_product(g, t, 3)

    def finish(g):
        pair(g, 1).wait_recv()

        def sum_of(s):
            r = pl.ds(pl.multiple_of(s * slot, 16), slot)
            cross(s).wait_recv()
            return r, (part[3, r, :].astype(f32) + core_got[1, r, :].astype(f32)
                       + x_got[r, :].astype(f32)).astype(bf)

        def body(s):
            r, value = sum_of(s)
            total[r, :] = value
            home(s).start()
        if g == 0:
            r, value = sum_of(0)
            back_rows[r, :] = value
        lo, hi = blocks(g)
        if hi > lo:
            loop(lo, hi, body)

    half = rows // 2

    def x_grads(h, lo, hi):
        r = slice(h * half, (h + 1) * half)

        def body(i):
            m = pl.ds(pl.multiple_of(i * 256, 256), 256)
            left = x_rows[r, m]
            for out, at in ((og, 0), (ou, ffe)):
                value = lax.dot_general(left, grads[r, at:at + ffe], FIRST,
                                        preferred_element_type=f32)
                if h:
                    value = value + out[m, :].astype(f32)
                out[m, :] = value.astype(bf)
        loop(lo, hi, body)

    def down_grads(h):
        r = slice(h * half, (h + 1) * half)
        for lo in range(0, ffe, 256):
            n = min(256, ffe - lo)
            value = lax.dot_general(hidden[r, lo:lo + n], c_rows[r, :], FIRST,
                                    preferred_element_type=f32)
            if h:
                value = value + od[lo:lo + n, :].astype(f32)
            od[lo:lo + n, :] = value.astype(bf)

    x_steps = width // 256
    loads[2].wait()
    each(0, arrive)
    each(1, arrive)
    turn(wd, wd_t)
    loads[3].wait()
    turn(wg, wg_t)
    loads[4].wait()
    turn(wu, wu_t)
    each(2, arrive)
    each(3, arrive)
    each(0, relay)
    each(1, relay)
    each(0, settled)
    each(1, settled)
    forward(0)
    backward(0)
    elementwise(0)
    each(4, arrive)
    each(2, relay)
    give_back(0)
    each(3, relay)
    each(5, arrive)
    each(2, settled)
    each(3, settled)
    forward(1)
    backward(1)
    elementwise(1)
    each(4, relay)
    give_back(1)
    x_grads(0, 0, x_steps // 2)
    each(6, arrive)
    each(5, relay)
    each(4, settled)
    each(5, settled)
    forward(2)
    each(7, arrive)
    backward(2)
    elementwise(2)
    give_back(2)
    finish(0)
    each(6, relay)
    x_grads(0, x_steps // 2, x_steps)
    each(7, relay)
    finish(1)
    down_grads(0)
    each(6, settled)
    each(7, settled)
    forward(3)
    backward(3)
    elementwise(3)
    sums = [rc(gate_all.at[t], gate_all.at[t], sum_send.at[o - 1], sum_recv.at[o - 1],
               me, lax.rem(t + o, 4)) for o in range(1, 4)]
    for copy in sums:
        copy.start()
    finish(2)
    give_back(3)
    x_grads(1, 0, x_steps // 2)
    for copy in sums:
        copy.wait_recv()
    gate_sum[...] = (gate_all[0] + gate_all[1]) + (gate_all[2] + gate_all[3])

    def sum_home(j):
        return rc(rblk(gate_sum, j, SUM_ROWS), rblk(back_gate, j, SUM_ROWS),
                  sumhome_send.at[j], sumhome_recv.at[j], flip(j), t)

    loop(1, groups, lambda j: sum_home(j).start())
    back_gate[0:SUM_ROWS, :] = gate_sum[0:SUM_ROWS, :]
    finish(3)
    x_grads(1, x_steps // 2, x_steps)
    down_grads(1)

    def landed(j):
        sum_home(j).wait_recv()
        home(j).wait_recv()

    def drain(j):
        for a in range(2):
            first(a, j).wait_send()
            to_core(a, j, t).wait_send()
            to_x(a, j, t).wait_send()
            to_core_again(a, j, x_peer).wait_send()
        sum_home(j).wait_send()
        home(j).wait_send()

    loop(1, groups, landed)
    loop(1, groups, drain)
    loop(0, groups, lambda s: cross(s).wait_send())
    for g in range(stages):
        for i in range(2):
            pair(g, i).wait_send()
    for copy in sums:
        copy.wait_send()


def collect_kernel(groups, slot, places, weights, back_rows, back_gate, og, ou, od,
                   grad_tokens, grad_gates, out_gate, out_up, out_down, out_sem):
    bf, f32 = jnp.bfloat16, jnp.float32
    outs = []
    for i, (src, dst) in enumerate(((og, out_gate), (ou, out_up), (od, out_down))):
        step = src.shape[0] // 2
        for h in range(2):
            copy = pltpu.make_async_copy(src.at[h * step:(h + 1) * step],
                                         dst.at[h * step:(h + 1) * step], out_sem.at[i, h])
            copy.start()
            outs.append(copy)
    tok_dev = places.shape[1]
    rows = groups * slot
    lanes = back_gate.shape[1]
    at = lax.broadcasted_iota(jnp.int32, (rows, tok_dev), 0)
    hit = (at == places[0:1, :]) | (at == places[1:2, :])
    grad_tokens[...] = lax.dot_general(
        jnp.where(hit, 1.0, 0.0).astype(bf), back_rows[...], FIRST,
        preferred_element_type=f32).astype(bf)
    sums = [jnp.zeros((1, tok_dev), f32), jnp.zeros((1, tok_dev), f32)]
    for j in range(groups):
        row = back_gate[j * SUM_ROWS:j * SUM_ROWS + 1, :]
        column = jnp.broadcast_to(row, (lanes, lanes)).T[0:slot, 0:1]
        here = lax.broadcasted_iota(jnp.int32, (slot, tok_dev), 0) + j * slot
        for k in range(2):
            sums[k] = sums[k] + jnp.sum(
                jnp.where(here == places[k:k + 1, :], column, 0.0), axis=0, keepdims=True)
    grad_gates[...] = jnp.concatenate(sums, axis=0) / weights[...].astype(f32)
    for copy in outs:
        copy.wait()


def on_device(tokens, cotangent, gate_weights, routes, w_gate, w_up, w_down):
    tok_dev, width = tokens.shape
    top_k = routes.shape[1]
    groups = lax.axis_size("ep")
    narrow = lax.axis_size("tp")
    capacity = 3 * top_k * tok_dev // (2 * groups)
    slot = -(-capacity // 16) * 16
    quarter = width // narrow
    ffe = w_gate.shape[2]
    rows = groups * slot
    lanes = -(-slot // 128) * 128
    stages = min(STAGES, groups)
    span = rows // stages
    vmem = pl.BlockSpec(memory_space=pltpu.VMEM)
    hbm = pl.BlockSpec(memory_space=pl.ANY)
    bf, f32 = jnp.bfloat16, jnp.float32
    dma = pltpu.SemaphoreType.DMA
    per = dma((groups,))
    twice = dma((2, groups))
    routes_t = routes.T
    weights_t = gate_weights.T
    og, ou, od, back_rows, back_gate, places = pl.pallas_call(
        functools.partial(expert_kernel, groups, slot, quarter),
        out_shape=(
            pltpu.VMEM((width, ffe), bf),
            pltpu.VMEM((width, ffe), bf),
            pltpu.VMEM((ffe, width), bf),
            pltpu.VMEM((rows, quarter), bf),
            pltpu.VMEM((groups * SUM_ROWS, lanes), f32),
            pltpu.VMEM((8, tok_dev), jnp.int32),
        ),
        in_specs=[vmem, vmem, hbm, hbm, hbm, hbm, hbm],
        out_specs=(vmem,) * 6,
        scratch_shapes=[
            pltpu.VMEM((tok_dev, width), bf),
            pltpu.VMEM((tok_dev, width), bf),
            pltpu.VMEM((rows, quarter), bf),
            pltpu.VMEM((rows, quarter), bf),
            pltpu.VMEM((min(NEAR, groups) * slot, quarter), bf),
            pltpu.VMEM((min(NEAR, groups) * slot, quarter), bf),
            pltpu.VMEM((rows, width), bf),
            pltpu.VMEM((rows, width), bf),
            pltpu.VMEM((width, ffe), bf),
            pltpu.VMEM((width, ffe), bf),
            pltpu.VMEM((ffe, width), bf),
            pltpu.VMEM((ffe, width), bf),
            pltpu.VMEM((ffe, width), bf),
            pltpu.VMEM((width, ffe), bf),
            pltpu.VMEM((span, ffe), f32),
            pltpu.VMEM((span, ffe), f32),
            pltpu.VMEM((span, ffe), f32),
            pltpu.VMEM((rows, ffe), bf),
            pltpu.VMEM((rows, 2 * ffe), bf),
            pltpu.VMEM((4, rows, quarter), bf),
            pltpu.VMEM((2, rows, quarter), bf),
            pltpu.VMEM((rows, quarter), bf),
            pltpu.VMEM((rows, quarter), bf),
            pltpu.VMEM((4, groups * SUM_ROWS, lanes), f32),
            pltpu.VMEM((groups * SUM_ROWS, lanes), f32),
            dma((5,)),
            twice, twice, twice, twice, twice, twice, twice, twice,
            dma((2, stages)), dma((2, stages)),
            per, per, per, per,
            dma((3,)), dma((3,)),
            per, per,
            dma((3,)),
        ],
        compiler_params=pltpu.CompilerParams(
            collective_id=0, has_side_effects=True, vmem_limit_bytes=52 * 2 ** 20),
        name="expert",
    )(routes_t, weights_t, tokens, cotangent, w_gate[0], w_up[0], w_down[0])
    held = [pltpu.with_memory_space_constraint(x, pltpu.VMEM)
            for x in (places, back_rows, back_gate, og, ou, od)]
    grad_tokens, grad_gates, grad_gate_w, grad_up_w, grad_down = pl.pallas_call(
        functools.partial(collect_kernel, groups, slot),
        out_shape=(
            jax.ShapeDtypeStruct((tok_dev, quarter), bf),
            jax.ShapeDtypeStruct((top_k, tok_dev), f32),
            jax.ShapeDtypeStruct((width, ffe), bf),
            jax.ShapeDtypeStruct((width, ffe), bf),
            jax.ShapeDtypeStruct((ffe, width), bf),
        ),
        in_specs=[vmem] * 7,
        out_specs=(vmem, vmem, hbm, hbm, hbm),
        scratch_shapes=[dma((3, 2))],
        compiler_params=pltpu.CompilerParams(vmem_limit_bytes=8 * 2 ** 20),
        name="collect",
    )(held[0], weights_t, *held[1:])
    return (grad_tokens, grad_gates.T, grad_gate_w[None], grad_up_w[None], grad_down[None])


def solution(mesh):
    in_specs = (
        P("ep", None),
        P("ep", None),
        P("ep", None),
        P("ep", None),
        P("ep", None, "tp"),
        P("ep", None, "tp"),
        P("ep", "tp", None),
    )
    out_specs = (
        P("ep", "tp"),
        P("ep", None),
        P("ep", None, "tp"),
        P("ep", None, "tp"),
        P("ep", "tp", None),
    )
    return jax.shard_map(
        on_device, mesh=mesh, in_specs=in_specs, out_specs=out_specs, check_vma=False
    )
```

```python
import functools

import jax
import jax.numpy as jnp
from jax import lax
from jax.experimental import pallas as pl
from jax.experimental.pallas import tpu as pltpu
from jax.sharding import PartitionSpec as P

MESH = pl.DeviceIdType.MESH
FIRST = (((0,), (0,)), ((), ()))
SUM_ROWS = 8
EIGHTHS = (0, 2, 4, 6, 8)
DIRECT = (2, 3)


def expert_kernel(groups, slot, quarter,
                  routes, weights, tokens, cotangent, w_gate, w_up, w_down,
                  og, ou, od, back_rows, back_gate, places, hidden, c_rows,
                  tok, cot, sent_x, sent_c, more_x, more_c, x_rows, wg, wu, wd, wg_t, wu_t, wd_t,
                  gate_pre, up_pre, back, grads,
                  part, core_got, x_got, total, gate_all, gate_sum,
                  load_sem, first_send, first_recv, core_send, core_recv,
                  x_send, x_recv, second_send, second_recv,
                  pair_send, pair_recv, cross_send, cross_recv, home_send, home_recv,
                  sum_send, sum_recv, sumhome_send, sumhome_recv, near_sem):
    me = lax.axis_index("ep")
    t = lax.axis_index("tp")
    core = lax.rem(t, 2)
    side = t // 2
    core_peer = side * 2 + (1 - core)
    x_peer = (1 - side) * 2 + core
    x_core_peer = (1 - side) * 2 + (1 - core)
    rows = groups * slot
    ffe = wg.shape[1]
    width = wg.shape[0]
    tok_dev = tok.shape[0]
    bf, f32 = jnp.bfloat16, jnp.float32
    bits = groups.bit_length() - 1
    stages = len(EIGHTHS) - 1
    edges = [e * groups // 8 for e in EIGHTHS]

    def rows_of(g):
        return slice(edges[g] * slot, edges[g + 1] * slot)

    def size_of(g):
        return (edges[g + 1] - edges[g]) * slot

    def flip(j):
        out = 0
        for b in range(bits):
            s = 1 << b
            out = out + s * lax.rem(lax.rem(me // s, 2) + lax.rem(j // s, 2), 2)
        return out

    def loop(lo, hi, body):
        def step(d, c):
            body(d)
            return c
        lax.fori_loop(lo, hi, step, 0)

    barrier = pltpu.get_barrier_semaphore()

    def greet(d):
        pl.semaphore_signal(barrier, inc=1, device_id=(lax.rem(me + d, groups), t),
                            device_id_type=MESH)

    loop(1, groups, greet)
    for o in range(1, 4):
        pl.semaphore_signal(barrier, inc=1, device_id=(me, lax.rem(t + o, 4)),
                            device_id_type=MESH)
    loads = [
        pltpu.make_async_copy(src, dst, load_sem.at[i])
        for i, (src, dst) in enumerate(((tokens, tok), (cotangent, cot), (w_down, wd),
                                        (w_gate, wg), (w_up, wu)))
    ]
    for load in loads:
        load.start()

    def rblk(ref, s, size=slot):
        return ref.at[pl.ds(pl.multiple_of(s * size, size if size < 16 else 16), size)]

    def cols(q):
        return pl.ds(pl.multiple_of(q * quarter, 128), quarter)

    def blk(ref, s, q):
        return ref.at[pl.ds(pl.multiple_of(s * slot, 16), slot), cols(q)]

    def rc(src, dst, ssem, rsem, ep, tp):
        return pltpu.make_async_remote_copy(
            src_ref=src, dst_ref=dst, send_sem=ssem, recv_sem=rsem,
            device_id=(ep, tp), device_id_type=MESH)

    is_end = 1 - (lax.rem(me // max(1, groups // 4), 3) + 1) // 2
    outer = is_end == 1
    inner = is_end == 0

    sent = (sent_x, sent_c)
    more = (more_x, more_c)
    full = (x_rows, c_rows)

    def first(a, j):
        return rc(rblk(sent[a], j), blk(full[a], j, t), first_send.at[a, j],
                  first_recv.at[a, j], flip(j), t)

    def to_core(a, j, q):
        return rc(blk(full[a], j, q), blk(full[a], j, q), core_send.at[a, j],
                  core_recv.at[a, j], me, core_peer)

    def to_x(a, j, q):
        return rc(blk(full[a], j, q), blk(full[a], j, q), x_send.at[a, j],
                  x_recv.at[a, j], me, x_peer)

    def direct(a, j):
        return rc(rblk(more[a], j - begin), blk(full[a], j, x_peer), x_send.at[a, j],
                  x_recv.at[a, j], flip(j), t)

    def to_core_again(a, j, q):
        return rc(blk(full[a], j, q), blk(full[a], j, q), second_send.at[a, j],
                  second_recv.at[a, j], me, core_peer)

    kinds = lax.broadcasted_iota(jnp.int32, (groups, tok_dev), 0)
    expert = jnp.bitwise_xor(kinds, me)
    hot = [(expert == routes[k:k + 1, :]).astype(f32) for k in range(2)]
    before = (lax.broadcasted_iota(jnp.int32, (tok_dev, tok_dev), 0)
              < lax.broadcasted_iota(jnp.int32, (tok_dev, tok_dev), 1)).astype(f32).astype(bf)
    earlier = jnp.dot(jnp.concatenate(hot, axis=0).astype(bf), before, preferred_element_type=f32)
    base = (kinds * slot).astype(f32)
    counts = (base + earlier[0:groups],
              base + earlier[groups:2 * groups] + jnp.sum(hot[0], axis=1, keepdims=True))
    place = [jnp.sum(hot[k] * counts[k], axis=0, keepdims=True).astype(jnp.int32)
             for k in range(2)]
    places[...] = jnp.concatenate(
        place + [jnp.full((6, tok_dev), -1, jnp.int32)], axis=0)
    share = [weights[k:k + 1, :].astype(f32) for k in range(2)]

    def picks(j):
        at = lax.broadcasted_iota(jnp.int32, (slot, tok_dev), 0) + j * slot
        hit = [at == places[k:k + 1, :] for k in range(2)]
        plain = jnp.where(hit[0] | hit[1], 1.0, 0.0).astype(bf)
        scaled = (jnp.where(hit[0], share[0], 0.0) + jnp.where(hit[1], share[1], 0.0)).astype(bf)
        return plain, scaled

    pl.semaphore_wait(barrier, groups + 2)
    loads[0].wait()
    loads[1].wait()

    def dispatch(j):
        plain, scaled = picks(j)
        r = pl.ds(pl.multiple_of(j * slot, 16), slot)
        sent_x[r, :] = jnp.dot(plain, tok[:, cols(t)], preferred_element_type=f32).astype(bf)
        first(0, j).start()
        sent_c[r, :] = jnp.dot(scaled, cot[:, cols(t)], preferred_element_type=f32).astype(bf)
        first(1, j).start()

    begin, end = DIRECT

    def dispatch_more(j):
        plain, scaled = picks(j)
        r = pl.ds(pl.multiple_of((j - begin) * slot, 16), slot)
        more_x[r, :] = jnp.dot(plain, tok[:, cols(x_peer)], preferred_element_type=f32).astype(bf)
        direct(0, j).start()
        more_c[r, :] = jnp.dot(scaled, cot[:, cols(x_peer)], preferred_element_type=f32).astype(bf)
        direct(1, j).start()

    far = edges[2]

    @pl.when(inner)
    def _():
        dispatch(far)
    loop(1, far, dispatch)
    loop(begin, end, dispatch_more)
    loop(far + (1 - is_end), groups, dispatch)
    plain, scaled = picks(0)
    x_rows[0:slot, :] = jnp.dot(plain, tok[...], preferred_element_type=f32).astype(bf)
    c_rows[0:slot, :] = jnp.dot(scaled, cot[...], preferred_element_type=f32).astype(bf)

    def blocks(g):
        return max(1, edges[g]), edges[g + 1]

    def arrive(a, j):
        first(a, j).wait_recv()
        to_x(a, j, t).start()
        to_core(a, j, t).start()

    def arrive_direct(a, j):
        first(a, j).wait_recv()
        to_core(a, j, t).start()

    def relay(a, j):
        to_x(a, j, x_peer).wait_recv()
        to_core_again(a, j, x_peer).start()

    def settled(a, j):
        to_core(a, j, core_peer).wait_recv()
        to_core_again(a, j, x_core_peer).wait_recv()

    def span_of(k):
        return max(1, k * groups // 8), (k + 1) * groups // 8

    def run(lo, hi, fn, tensors):
        def body(j):
            for a in tensors:
                fn(a, j)
        if hi > lo:
            loop(lo, hi, body)

    def each(k, fn, tensors=(0, 1)):
        lo, hi = span_of(k)
        if fn is arrive:
            run(lo, min(hi, begin), arrive, tensors)
            run(max(lo, begin), min(hi, end), arrive_direct, tensors)
            lo = max(lo, end)
        run(lo, hi, fn, tensors)

    def turn(src, dst):
        for lo in range(0, src.shape[0], 128):
            n = min(128, src.shape[0] - lo)
            dst[:, lo:lo + n] = src[lo:lo + n, :].T

    def forward(g):
        r, n = rows_of(g), size_of(g)
        gate_pre[0:n, :] = jnp.dot(x_rows[r, :], wg[...], preferred_element_type=f32)
        up_pre[0:n, :] = jnp.dot(x_rows[r, :], wu[...], preferred_element_type=f32)

    def backward(g):
        r, n = rows_of(g), size_of(g)
        back[0:n, :] = jnp.dot(c_rows[r, :], wd_t[...], preferred_element_type=f32)

    lanes = gate_all.shape[2]

    def elementwise(g):
        def body(i):
            r = pl.ds(pl.multiple_of(i * slot, 16), slot)
            w = pl.ds(pl.multiple_of((edges[g] + i) * slot, 16), slot)
            summed = jnp.zeros((slot, 128), f32)
            for lo in range(0, ffe, 128):
                v = gate_pre[r, lo:lo + 128]
                u = up_pre[r, lo:lo + 128]
                b = back[r, lo:lo + 128]
                logistic = jax.nn.sigmoid(v)
                act = v * logistic
                h = (act * u).astype(bf)
                hidden[w, lo:lo + 128] = h
                summed = summed + h.astype(f32) * b
                grads[w, lo:lo + 128] = (b * u * logistic * (1.0 + v * (1.0 - logistic))).astype(bf)
                grads[w, ffe + lo:ffe + lo + 128] = (b * act).astype(bf)
            if lanes > slot:
                summed = jnp.concatenate([summed, jnp.zeros((lanes - slot, 128), f32)], axis=0)
            row = jnp.sum(summed.T, axis=0, keepdims=True)
            gate_all[t, pl.ds(edges[g] + i, 1), :] = row
        loop(0, edges[g + 1] - edges[g], body)

    def row_product(g, q, i):
        r = rows_of(g)
        value = jnp.dot(grads[r, 0:ffe], wg_t[:, cols(q)], preferred_element_type=f32)
        value = value + jnp.dot(grads[r, ffe:2 * ffe], wu_t[:, cols(q)],
                                preferred_element_type=f32)
        part[i, r, :] = value.astype(bf)

    def pair(g, i):
        r = pl.ds(edges[g] * slot, size_of(g))
        return rc(part.at[i, r], core_got.at[i, r], pair_send.at[i, g], pair_recv.at[i, g],
                  me, core_peer)

    def cross(s):
        return rc(rblk(part.at[2], s), rblk(x_got, s), cross_send.at[s], cross_recv.at[s],
                  me, x_peer)

    def home(j):
        return rc(rblk(total, j), rblk(back_rows, j), home_send.at[j], home_recv.at[j],
                  flip(j), t)

    def products(g):
        row_product(g, x_core_peer, 0)
        pair(g, 0).start()
        row_product(g, x_peer, 2)
        row_product(g, core_peer, 1)
        pair(g, 1).start()
        row_product(g, t, 3)

    def crosses(g):
        pair(g, 0).wait_recv()

        def add_cross(s):
            r = pl.ds(pl.multiple_of(s * slot, 16), slot)
            part[2, r, :] = (part[2, r, :].astype(f32) + core_got[0, r, :].astype(f32)).astype(bf)
            cross(s).start()
        loop(0, edges[g + 1] - edges[g], lambda i: add_cross(edges[g + 1] - 1 - i))

    def give_back(g):
        row_product(g, x_core_peer, 0)
        pair(g, 0).start()
        row_product(g, x_peer, 2)
        crosses(g)
        row_product(g, core_peer, 1)
        pair(g, 1).start()
        row_product(g, t, 3)

    def finish(g):
        pair(g, 1).wait_recv()

        def sum_of(s):
            r = pl.ds(pl.multiple_of(s * slot, 16), slot)
            cross(s).wait_recv()
            return r, (part[3, r, :].astype(f32) + core_got[1, r, :].astype(f32)
                       + x_got[r, :].astype(f32)).astype(bf)

        def body(s):
            r, value = sum_of(s)
            total[r, :] = value
            home(s).start()
        lo, hi = blocks(g)
        if hi > lo:
            loop(lo, hi, body)
        if g == 0:
            r, value = sum_of(0)
            back_rows[r, :] = value

    def x_grads(lo, hi):
        def body(i):
            m = pl.ds(pl.multiple_of(i * 256, 256), 256)
            left = x_rows[:, m]
            og[m, :] = lax.dot_general(left, grads[:, 0:ffe], FIRST,
                                       preferred_element_type=f32).astype(bf)
            ou[m, :] = lax.dot_general(left, grads[:, ffe:2 * ffe], FIRST,
                                       preferred_element_type=f32).astype(bf)
        loop(lo, hi, body)

    half = rows // 2

    def down_grads():
        for lo in range(0, ffe, 256):
            n = min(256, ffe - lo)
            od[lo:lo + n, :] = lax.dot_general(
                hidden[0:half, lo:lo + n], c_rows[0:half, :], FIRST,
                preferred_element_type=f32).astype(bf)


    x_steps = width // 256
    loads[2].wait()
    each(0, arrive)
    each(1, arrive)
    turn(wd, wd_t)
    loads[3].wait()
    turn(wg, wg_t)
    loads[4].wait()
    turn(wu, wu_t)
    each(0, relay)
    each(1, relay)
    each(0, settled)
    each(1, settled)
    forward(0)
    backward(0)
    elementwise(0)

    @pl.when(inner)
    def _():
        each(2, arrive)
        each(3, arrive)
    products(0)

    @pl.when(outer)
    def _():
        crosses(0)
        each(2, arrive)
        each(3, arrive)
    each(4, arrive)

    @pl.when(inner)
    def _():
        crosses(0)
    each(2, relay)

    @pl.when(outer)
    def _():
        each(5, arrive)
    each(3, relay)
    each(2, settled)
    each(3, settled)
    forward(1)

    @pl.when(inner)
    def _():
        each(5, arrive)
    backward(1)
    elementwise(1)
    each(4, relay)
    products(1)
    each(6, arrive)

    @pl.when(outer)
    def _():
        each(7, arrive)
    each(5, relay)
    each(4, settled)
    each(5, settled)
    forward(2)
    backward(2)
    elementwise(2)

    @pl.when(inner)
    def _():
        each(7, arrive)
    give_back(2)
    crosses(1)
    finish(0)
    each(6, relay)
    each(7, relay, (0,))
    down_grads()
    each(6, settled)
    each(7, settled, (0,))
    forward(3)
    each(7, relay, (1,))
    each(7, settled, (1,))
    backward(3)
    elementwise(3)
    sums = [rc(gate_all.at[t], gate_all.at[t], sum_send.at[o - 1], sum_recv.at[o - 1],
               me, lax.rem(t + o, 4)) for o in range(1, 4)]
    for copy in sums:
        copy.start()
    finish(2)
    give_back(3)
    finish(1)
    x_grads(0, x_steps // 4)
    for copy in sums:
        copy.wait_recv()
    gate_rows = (gate_all[0] + gate_all[1]) + (gate_all[2] + gate_all[3])
    for j in range(groups):
        gate_sum[j * SUM_ROWS:(j + 1) * SUM_ROWS, :] = jnp.broadcast_to(
            gate_rows[j:j + 1, :], (SUM_ROWS, lanes))

    def sum_home(j):
        return rc(rblk(gate_sum, j, SUM_ROWS), rblk(back_gate, j, SUM_ROWS),
                  sumhome_send.at[j], sumhome_recv.at[j], flip(j), t)

    loop(1, groups, lambda j: sum_home(j).start())
    back_gate[0:SUM_ROWS, :] = gate_sum[0:SUM_ROWS, :]
    x_grads(x_steps // 4, x_steps // 2)
    finish(3)
    x_grads(x_steps // 2, x_steps)

    def landed(j):
        sum_home(j).wait_recv()
        home(j).wait_recv()

    def drain(j):
        for a in range(2):
            first(a, j).wait_send()
            to_core(a, j, t).wait_send()
            to_x(a, j, t).wait_send()
            to_core_again(a, j, x_peer).wait_send()
        sum_home(j).wait_send()
        home(j).wait_send()

    loop(1, groups, landed)
    loop(1, groups, drain)
    loop(0, groups, lambda s: cross(s).wait_send())
    for g in range(stages):
        for i in range(2):
            pair(g, i).wait_send()
    for copy in sums:
        copy.wait_send()


def collect_kernel(groups, slot, places, weights, back_rows, back_gate, hidden, c_rows, og, ou, od,
                   grad_tokens, grad_gates, out_gate, out_up, out_down, summed, out_sem):
    bf, f32 = jnp.bfloat16, jnp.float32
    outs = []

    def put(src, dst, i, h, lo, n):
        copy = pltpu.make_async_copy(src.at[lo:lo + n], dst.at[lo:lo + n], out_sem.at[i, h])
        copy.start()
        outs.append(copy)

    for i, (src, dst) in enumerate(((og, out_gate), (ou, out_up))):
        step = src.shape[0] // 4
        for h in range(4):
            put(src, dst, i, h, h * step, step)
    half = groups * slot // 2
    ffe = hidden.shape[1]
    step = -(-ffe // 4 // 128) * 128
    for h, lo in enumerate(range(0, ffe, step)):
        n = min(step, ffe - lo)
        value = lax.dot_general(hidden[half:, lo:lo + n], c_rows[half:, :], FIRST,
                                preferred_element_type=f32)
        summed[lo:lo + n, :] = (value + od[lo:lo + n, :].astype(f32)).astype(bf)
        put(summed, out_down, 2, h, lo, n)
    tok_dev = places.shape[1]
    rows = groups * slot
    lanes = back_gate.shape[1]
    at = lax.broadcasted_iota(jnp.int32, (rows, tok_dev), 0)
    hit = (at == places[0:1, :]) | (at == places[1:2, :])
    grad_tokens[...] = lax.dot_general(
        jnp.where(hit, 1.0, 0.0).astype(bf), back_rows[...], FIRST,
        preferred_element_type=f32).astype(bf)
    sums = [jnp.zeros((1, tok_dev), f32), jnp.zeros((1, tok_dev), f32)]
    for j in range(groups):
        row = back_gate[j * SUM_ROWS:j * SUM_ROWS + 1, :]
        column = jnp.broadcast_to(row, (lanes, lanes)).T[0:slot, 0:1]
        here = lax.broadcasted_iota(jnp.int32, (slot, tok_dev), 0) + j * slot
        for k in range(2):
            sums[k] = sums[k] + jnp.sum(
                jnp.where(here == places[k:k + 1, :], column, 0.0), axis=0, keepdims=True)
    grad_gates[...] = jnp.concatenate(sums, axis=0) / weights[...].astype(f32)
    for copy in outs:
        copy.wait()


def on_device(tokens, cotangent, gate_weights, routes, w_gate, w_up, w_down):
    tok_dev, width = tokens.shape
    top_k = routes.shape[1]
    groups = lax.axis_size("ep")
    narrow = lax.axis_size("tp")
    capacity = 3 * top_k * tok_dev // (2 * groups)
    slot = -(-capacity // 16) * 16
    quarter = width // narrow
    ffe = w_gate.shape[2]
    rows = groups * slot
    lanes = -(-slot // 128) * 128
    stages = len(EIGHTHS) - 1
    span = max(b - a for a, b in zip(EIGHTHS, EIGHTHS[1:])) * groups // 8 * slot
    vmem = pl.BlockSpec(memory_space=pltpu.VMEM)
    hbm = pl.BlockSpec(memory_space=pl.ANY)
    bf, f32 = jnp.bfloat16, jnp.float32
    dma = pltpu.SemaphoreType.DMA
    per = dma((groups,))
    twice = dma((2, groups))
    routes_t = routes.T
    weights_t = gate_weights.T
    og, ou, od, back_rows, back_gate, places, hidden, c_rows = pl.pallas_call(
        functools.partial(expert_kernel, groups, slot, quarter),
        out_shape=(
            pltpu.VMEM((width, ffe), bf),
            pltpu.VMEM((width, ffe), bf),
            pltpu.VMEM((ffe, width), bf),
            pltpu.VMEM((rows, quarter), bf),
            pltpu.VMEM((groups * SUM_ROWS, lanes), f32),
            pltpu.VMEM((8, tok_dev), jnp.int32),
            pltpu.VMEM((rows, ffe), bf),
            pltpu.VMEM((rows, width), bf),
        ),
        in_specs=[vmem, vmem, hbm, hbm, hbm, hbm, hbm],
        out_specs=(vmem,) * 8,
        scratch_shapes=[
            pltpu.VMEM((tok_dev, width), bf),
            pltpu.VMEM((tok_dev, width), bf),
            pltpu.VMEM((rows, quarter), bf),
            pltpu.VMEM((rows, quarter), bf),
            pltpu.VMEM(((DIRECT[1] - DIRECT[0]) * slot, quarter), bf),
            pltpu.VMEM(((DIRECT[1] - DIRECT[0]) * slot, quarter), bf),
            pltpu.VMEM((rows, width), bf),
            pltpu.VMEM((width, ffe), bf),
            pltpu.VMEM((width, ffe), bf),
            pltpu.VMEM((ffe, width), bf),
            pltpu.VMEM((ffe, width), bf),
            pltpu.VMEM((ffe, width), bf),
            pltpu.VMEM((width, ffe), bf),
            pltpu.VMEM((span, ffe), f32),
            pltpu.VMEM((span, ffe), f32),
            pltpu.VMEM((span, ffe), f32),
            pltpu.VMEM((rows, 2 * ffe), bf),
            pltpu.VMEM((4, rows, quarter), bf),
            pltpu.VMEM((2, rows, quarter), bf),
            pltpu.VMEM((rows, quarter), bf),
            pltpu.VMEM((rows, quarter), bf),
            pltpu.VMEM((4, groups, lanes), f32),
            pltpu.VMEM((groups * SUM_ROWS, lanes), f32),
            dma((5,)),
            twice, twice, twice, twice, twice, twice, twice, twice,
            dma((2, stages)), dma((2, stages)),
            per, per, per, per,
            dma((3,)), dma((3,)),
            per, per,
            dma((3,)),
        ],
        compiler_params=pltpu.CompilerParams(
            collective_id=0, has_side_effects=True, vmem_limit_bytes=46 * 2 ** 20),
        name="expert",
    )(routes_t, weights_t, tokens, cotangent, w_gate[0], w_up[0], w_down[0])
    held = [pltpu.with_memory_space_constraint(x, pltpu.VMEM)
            for x in (places, back_rows, back_gate, hidden, c_rows, og, ou, od)]
    grad_tokens, grad_gates, grad_gate_w, grad_up_w, grad_down = pl.pallas_call(
        functools.partial(collect_kernel, groups, slot),
        out_shape=(
            jax.ShapeDtypeStruct((tok_dev, quarter), bf),
            jax.ShapeDtypeStruct((top_k, tok_dev), f32),
            jax.ShapeDtypeStruct((width, ffe), bf),
            jax.ShapeDtypeStruct((width, ffe), bf),
            jax.ShapeDtypeStruct((ffe, width), bf),
        ),
        in_specs=[vmem] * 9,
        out_specs=(vmem, vmem, hbm, hbm, hbm),
        scratch_shapes=[pltpu.VMEM((ffe, width), bf), dma((3, 4))],
        compiler_params=pltpu.CompilerParams(vmem_limit_bytes=12 * 2 ** 20),
        name="collect",
    )(held[0], weights_t, *held[1:])
    return (grad_tokens, grad_gates.T, grad_gate_w[None], grad_up_w[None], grad_down[None])


def solution(mesh):
    in_specs = (
        P("ep", None),
        P("ep", None),
        P("ep", None),
        P("ep", None),
        P("ep", None, "tp"),
        P("ep", None, "tp"),
        P("ep", "tp", None),
    )
    out_specs = (
        P("ep", "tp"),
        P("ep", None),
        P("ep", None, "tp"),
        P("ep", None, "tp"),
        P("ep", "tp", None),
    )
    return jax.shard_map(
        on_device, mesh=mesh, in_specs=in_specs, out_specs=out_specs, check_vma=False
    )
```

```python
import functools

import jax
import jax.numpy as jnp
from jax import lax
from jax.experimental import pallas as pl
from jax.experimental.pallas import tpu as pltpu
from jax.sharding import PartitionSpec as P

MESH = pl.DeviceIdType.MESH
FIRST = (((0,), (0,)), ((), ()))
SUM_ROWS = 8
EIGHTHS = (0, 2, 4, 6, 8)
DIRECT = (2, 3)


def expert_kernel(groups, slot, quarter,
                  routes, weights, tokens, cotangent, w_gate, w_up, w_down,
                  og, ou, od, back_rows, back_gate, places, hidden, c_rows,
                  tok, cot, sent_x, sent_c, more_x, more_c, x_rows, wg, wu, wd, wg_t, wu_t, wd_t,
                  gate_pre, up_pre, back, grads,
                  part, core_got, x_got, total, gate_all, gate_sum,
                  load_sem, first_send, first_recv, core_send, core_recv,
                  x_send, x_recv, second_send, second_recv,
                  pair_send, pair_recv, cross_send, cross_recv, home_send, home_recv,
                  sum_send, sum_recv, sumhome_send, sumhome_recv, near_sem):
    me = lax.axis_index("ep")
    t = lax.axis_index("tp")
    core = lax.rem(t, 2)
    side = t // 2
    core_peer = side * 2 + (1 - core)
    x_peer = (1 - side) * 2 + core
    x_core_peer = (1 - side) * 2 + (1 - core)
    rows = groups * slot
    ffe = wg.shape[1]
    width = wg.shape[0]
    tok_dev = tok.shape[0]
    bf, f32 = jnp.bfloat16, jnp.float32
    bits = groups.bit_length() - 1
    stages = len(EIGHTHS) - 1
    edges = [e * groups // 8 for e in EIGHTHS]

    def rows_of(g):
        return slice(edges[g] * slot, edges[g + 1] * slot)

    def size_of(g):
        return (edges[g + 1] - edges[g]) * slot

    def flip(j):
        out = 0
        for b in range(bits):
            s = 1 << b
            out = out + s * lax.rem(lax.rem(me // s, 2) + lax.rem(j // s, 2), 2)
        return out

    def loop(lo, hi, body):
        def step(d, c):
            body(d)
            return c
        lax.fori_loop(lo, hi, step, 0)

    barrier = pltpu.get_barrier_semaphore()

    def greet(d):
        pl.semaphore_signal(barrier, inc=1, device_id=(lax.rem(me + d, groups), t),
                            device_id_type=MESH)

    loop(1, groups, greet)
    for o in range(1, 4):
        pl.semaphore_signal(barrier, inc=1, device_id=(me, lax.rem(t + o, 4)),
                            device_id_type=MESH)
    loads = [
        pltpu.make_async_copy(src, dst, load_sem.at[i])
        for i, (src, dst) in enumerate(((tokens, tok), (cotangent, cot), (w_down, wd),
                                        (w_gate, wg), (w_up, wu)))
    ]
    for load in loads:
        load.start()

    def rblk(ref, s, size=slot):
        return ref.at[pl.ds(pl.multiple_of(s * size, size if size < 16 else 16), size)]

    def cols(q):
        return pl.ds(pl.multiple_of(q * quarter, 128), quarter)

    def blk(ref, s, q):
        return ref.at[pl.ds(pl.multiple_of(s * slot, 16), slot), cols(q)]

    def rc(src, dst, ssem, rsem, ep, tp):
        return pltpu.make_async_remote_copy(
            src_ref=src, dst_ref=dst, send_sem=ssem, recv_sem=rsem,
            device_id=(ep, tp), device_id_type=MESH)

    is_end = 1 - (lax.rem(me // max(1, groups // 4), 3) + 1) // 2
    outer = is_end == 1
    inner = is_end == 0

    sent = (sent_x, sent_c)
    more = (more_x, more_c)
    full = (x_rows, c_rows)

    def first(a, j):
        return rc(rblk(sent[a], j), blk(full[a], j, t), first_send.at[a, j],
                  first_recv.at[a, j], flip(j), t)

    def to_core(a, j, q):
        return rc(blk(full[a], j, q), blk(full[a], j, q), core_send.at[a, j],
                  core_recv.at[a, j], me, core_peer)

    def to_x(a, j, q):
        return rc(blk(full[a], j, q), blk(full[a], j, q), x_send.at[a, j],
                  x_recv.at[a, j], me, x_peer)

    def direct(a, j):
        return rc(rblk(more[a], j - begin), blk(full[a], j, x_peer), x_send.at[a, j],
                  x_recv.at[a, j], flip(j), t)

    def to_core_again(a, j, q):
        return rc(blk(full[a], j, q), blk(full[a], j, q), second_send.at[a, j],
                  second_recv.at[a, j], me, core_peer)

    kinds = lax.broadcasted_iota(jnp.int32, (groups, tok_dev), 0)
    expert = jnp.bitwise_xor(kinds, me)
    hot = [(expert == routes[k:k + 1, :]).astype(f32) for k in range(2)]
    before = (lax.broadcasted_iota(jnp.int32, (tok_dev, tok_dev), 0)
              < lax.broadcasted_iota(jnp.int32, (tok_dev, tok_dev), 1)).astype(f32).astype(bf)
    earlier = jnp.dot(jnp.concatenate(hot, axis=0).astype(bf), before, preferred_element_type=f32)
    base = (kinds * slot).astype(f32)
    counts = (base + earlier[0:groups],
              base + earlier[groups:2 * groups] + jnp.sum(hot[0], axis=1, keepdims=True))
    place = [jnp.sum(hot[k] * counts[k], axis=0, keepdims=True).astype(jnp.int32)
             for k in range(2)]
    places[...] = jnp.concatenate(
        place + [jnp.full((6, tok_dev), -1, jnp.int32)], axis=0)
    share = [weights[k:k + 1, :].astype(f32) for k in range(2)]

    def picks(j):
        at = lax.broadcasted_iota(jnp.int32, (slot, tok_dev), 0) + j * slot
        hit = [at == places[k:k + 1, :] for k in range(2)]
        plain = jnp.where(hit[0] | hit[1], 1.0, 0.0).astype(bf)
        scaled = (jnp.where(hit[0], share[0], 0.0) + jnp.where(hit[1], share[1], 0.0)).astype(bf)
        return plain, scaled

    pl.semaphore_wait(barrier, groups + 2)
    loads[0].wait()
    loads[1].wait()

    def dispatch(j):
        plain, scaled = picks(j)
        r = pl.ds(pl.multiple_of(j * slot, 16), slot)
        sent_x[r, :] = jnp.dot(plain, tok[:, cols(t)], preferred_element_type=f32).astype(bf)
        first(0, j).start()
        sent_c[r, :] = jnp.dot(scaled, cot[:, cols(t)], preferred_element_type=f32).astype(bf)
        first(1, j).start()

    begin, end = DIRECT

    def dispatch_more(j):
        plain, scaled = picks(j)
        r = pl.ds(pl.multiple_of((j - begin) * slot, 16), slot)
        more_x[r, :] = jnp.dot(plain, tok[:, cols(x_peer)], preferred_element_type=f32).astype(bf)
        direct(0, j).start()
        more_c[r, :] = jnp.dot(scaled, cot[:, cols(x_peer)], preferred_element_type=f32).astype(bf)
        direct(1, j).start()

    far = edges[2]

    @pl.when(inner)
    def _():
        dispatch(far)
    loop(1, far, dispatch)
    loop(begin, end, dispatch_more)
    loop(far + (1 - is_end), groups, dispatch)
    plain, scaled = picks(0)
    x_rows[0:slot, :] = jnp.dot(plain, tok[...], preferred_element_type=f32).astype(bf)
    c_rows[0:slot, :] = jnp.dot(scaled, cot[...], preferred_element_type=f32).astype(bf)

    def blocks(g):
        return max(1, edges[g]), edges[g + 1]

    def arrive(a, j):
        first(a, j).wait_recv()
        to_x(a, j, t).start()
        to_core(a, j, t).start()

    def arrive_direct(a, j):
        first(a, j).wait_recv()
        to_core(a, j, t).start()

    def relay(a, j):
        to_x(a, j, x_peer).wait_recv()
        to_core_again(a, j, x_peer).start()

    def settled(a, j):
        to_core(a, j, core_peer).wait_recv()
        to_core_again(a, j, x_core_peer).wait_recv()

    def span_of(k):
        return max(1, k * groups // 8), (k + 1) * groups // 8

    def run(lo, hi, fn, tensors):
        def body(j):
            for a in tensors:
                fn(a, j)
        if hi > lo:
            loop(lo, hi, body)

    def each(k, fn, tensors=(0, 1)):
        lo, hi = span_of(k)
        if fn is arrive:
            run(lo, min(hi, begin), arrive, tensors)
            run(max(lo, begin), min(hi, end), arrive_direct, tensors)
            lo = max(lo, end)
        run(lo, hi, fn, tensors)

    def turn(src, dst):
        for lo in range(0, src.shape[0], 128):
            n = min(128, src.shape[0] - lo)
            dst[:, lo:lo + n] = src[lo:lo + n, :].T

    def forward(g):
        r, n = rows_of(g), size_of(g)
        gate_pre[0:n, :] = jnp.dot(x_rows[r, :], wg[...], preferred_element_type=f32)
        up_pre[0:n, :] = jnp.dot(x_rows[r, :], wu[...], preferred_element_type=f32)

    def backward(g):
        r, n = rows_of(g), size_of(g)
        back[0:n, :] = jnp.dot(c_rows[r, :], wd_t[...], preferred_element_type=f32)

    lanes = gate_all.shape[2]

    def elementwise(g):
        def body(i):
            r = pl.ds(pl.multiple_of(i * slot, 16), slot)
            w = pl.ds(pl.multiple_of((edges[g] + i) * slot, 16), slot)
            summed = jnp.zeros((slot, 128), f32)
            for lo in range(0, ffe, 128):
                v = gate_pre[r, lo:lo + 128]
                u = up_pre[r, lo:lo + 128]
                b = back[r, lo:lo + 128]
                logistic = jax.nn.sigmoid(v)
                act = v * logistic
                h = (act * u).astype(bf)
                hidden[w, lo:lo + 128] = h
                summed = summed + h.astype(f32) * b
                grads[w, lo:lo + 128] = (b * u * logistic * (1.0 + v * (1.0 - logistic))).astype(bf)
                grads[w, ffe + lo:ffe + lo + 128] = (b * act).astype(bf)
            if lanes > slot:
                summed = jnp.concatenate([summed, jnp.zeros((lanes - slot, 128), f32)], axis=0)
            row = jnp.sum(summed.T, axis=0, keepdims=True)
            gate_all[t, pl.ds(edges[g] + i, 1), :] = row
        loop(0, edges[g + 1] - edges[g], body)

    def row_product(g, q, i):
        r = rows_of(g)
        value = jnp.dot(grads[r, 0:ffe], wg_t[:, cols(q)], preferred_element_type=f32)
        value = value + jnp.dot(grads[r, ffe:2 * ffe], wu_t[:, cols(q)],
                                preferred_element_type=f32)
        part[i, r, :] = value.astype(bf)

    def pair(g, i):
        r = pl.ds(edges[g] * slot, size_of(g))
        return rc(part.at[i, r], core_got.at[i, r], pair_send.at[i, g], pair_recv.at[i, g],
                  me, core_peer)

    def cross(s):
        return rc(rblk(part.at[2], s), rblk(x_got, s), cross_send.at[s], cross_recv.at[s],
                  me, x_peer)

    def home(j):
        return rc(rblk(total, j), rblk(back_rows, j), home_send.at[j], home_recv.at[j],
                  flip(j), t)

    def products(g):
        row_product(g, x_core_peer, 0)
        pair(g, 0).start()
        row_product(g, x_peer, 2)
        row_product(g, core_peer, 1)
        pair(g, 1).start()
        row_product(g, t, 3)

    def crosses(g):
        pair(g, 0).wait_recv()

        def add_cross(s):
            r = pl.ds(pl.multiple_of(s * slot, 16), slot)
            part[2, r, :] = (part[2, r, :].astype(f32) + core_got[0, r, :].astype(f32)).astype(bf)
            cross(s).start()
        loop(0, edges[g + 1] - edges[g], lambda i: add_cross(edges[g + 1] - 1 - i))

    def give_back(g):
        row_product(g, x_core_peer, 0)
        pair(g, 0).start()
        row_product(g, x_peer, 2)
        row_product(g, core_peer, 1)
        pair(g, 1).start()
        crosses(g)
        row_product(g, t, 3)

    def finish(g):
        pair(g, 1).wait_recv()

        def sum_of(s):
            r = pl.ds(pl.multiple_of(s * slot, 16), slot)
            cross(s).wait_recv()
            return r, (part[3, r, :].astype(f32) + core_got[1, r, :].astype(f32)
                       + x_got[r, :].astype(f32)).astype(bf)

        def body(s):
            r, value = sum_of(s)
            total[r, :] = value
            home(s).start()
        lo, hi = blocks(g)
        if hi > lo:
            loop(lo, hi, body)
        if g == 0:
            r, value = sum_of(0)
            back_rows[r, :] = value

    def x_grads(lo, hi):
        def body(i):
            m = pl.ds(pl.multiple_of(i * 256, 256), 256)
            left = x_rows[:, m]
            og[m, :] = lax.dot_general(left, grads[:, 0:ffe], FIRST,
                                       preferred_element_type=f32).astype(bf)
            ou[m, :] = lax.dot_general(left, grads[:, ffe:2 * ffe], FIRST,
                                       preferred_element_type=f32).astype(bf)
        loop(lo, hi, body)

    half = rows // 2

    def down_grads():
        for lo in range(0, ffe, 256):
            n = min(256, ffe - lo)
            od[lo:lo + n, :] = lax.dot_general(
                hidden[0:half, lo:lo + n], c_rows[0:half, :], FIRST,
                preferred_element_type=f32).astype(bf)


    x_steps = width // 256
    loads[2].wait()
    each(0, arrive)
    each(1, arrive)
    turn(wd, wd_t)
    loads[3].wait()
    turn(wg, wg_t)
    loads[4].wait()
    turn(wu, wu_t)
    each(0, relay)
    each(1, relay)
    each(0, settled)
    each(1, settled)
    forward(0)
    backward(0)
    elementwise(0)

    @pl.when(inner)
    def _():
        each(2, arrive)
        each(3, arrive)
    products(0)

    @pl.when(outer)
    def _():
        crosses(0)
        each(2, arrive)
        each(3, arrive)
    each(4, arrive)

    @pl.when(inner)
    def _():
        crosses(0)
    each(2, relay)

    @pl.when(outer)
    def _():
        each(5, arrive)
    each(3, relay)
    each(2, settled)
    each(3, settled)
    forward(1)

    @pl.when(inner)
    def _():
        each(5, arrive)
    backward(1)
    elementwise(1)
    each(4, relay)
    products(1)
    each(6, arrive)

    @pl.when(outer)
    def _():
        each(7, arrive)
    each(5, relay)
    each(4, settled)
    each(5, settled)
    forward(2)
    backward(2)
    elementwise(2)

    @pl.when(inner)
    def _():
        each(7, arrive)
    give_back(2)
    crosses(1)
    finish(0)
    each(6, relay)
    each(7, relay, (0,))
    down_grads()
    each(6, settled)
    each(7, settled, (0,))
    forward(3)
    each(7, relay, (1,))
    each(7, settled, (1,))
    backward(3)
    elementwise(3)
    sums = [rc(gate_all.at[t], gate_all.at[t], sum_send.at[o - 1], sum_recv.at[o - 1],
               me, lax.rem(t + o, 4)) for o in range(1, 4)]
    for copy in sums:
        copy.start()
    finish(2)
    give_back(3)
    finish(1)
    x_grads(0, x_steps // 4)
    for copy in sums:
        copy.wait_recv()
    gate_rows = (gate_all[0] + gate_all[1]) + (gate_all[2] + gate_all[3])
    for j in range(groups):
        gate_sum[j * SUM_ROWS:(j + 1) * SUM_ROWS, :] = jnp.broadcast_to(
            gate_rows[j:j + 1, :], (SUM_ROWS, lanes))

    def sum_home(j):
        return rc(rblk(gate_sum, j, SUM_ROWS), rblk(back_gate, j, SUM_ROWS),
                  sumhome_send.at[j], sumhome_recv.at[j], flip(j), t)

    loop(1, groups, lambda j: sum_home(j).start())
    back_gate[0:SUM_ROWS, :] = gate_sum[0:SUM_ROWS, :]
    x_grads(x_steps // 4, x_steps // 2)
    finish(3)
    x_grads(x_steps // 2, x_steps)

    def landed(j):
        sum_home(j).wait_recv()
        home(j).wait_recv()

    def drain(j):
        for a in range(2):
            first(a, j).wait_send()
            to_core(a, j, t).wait_send()
            to_x(a, j, t).wait_send()
            to_core_again(a, j, x_peer).wait_send()
        sum_home(j).wait_send()
        home(j).wait_send()

    loop(1, groups, landed)
    loop(1, groups, drain)
    loop(0, groups, lambda s: cross(s).wait_send())
    for g in range(stages):
        for i in range(2):
            pair(g, i).wait_send()
    for copy in sums:
        copy.wait_send()


def collect_kernel(groups, slot, places, weights, back_rows, back_gate, hidden, c_rows, og, ou, od,
                   grad_tokens, grad_gates, out_gate, out_up, out_down, summed, out_sem):
    bf, f32 = jnp.bfloat16, jnp.float32
    outs = []

    def put(src, dst, i, h, lo, n):
        copy = pltpu.make_async_copy(src.at[lo:lo + n], dst.at[lo:lo + n], out_sem.at[i, h])
        copy.start()
        outs.append(copy)

    for i, (src, dst) in enumerate(((og, out_gate), (ou, out_up))):
        step = src.shape[0] // 4
        for h in range(4):
            put(src, dst, i, h, h * step, step)
    half = groups * slot // 2
    ffe = hidden.shape[1]
    step = -(-ffe // 4 // 128) * 128
    for h, lo in enumerate(range(0, ffe, step)):
        n = min(step, ffe - lo)
        value = lax.dot_general(hidden[half:, lo:lo + n], c_rows[half:, :], FIRST,
                                preferred_element_type=f32)
        summed[lo:lo + n, :] = (value + od[lo:lo + n, :].astype(f32)).astype(bf)
        put(summed, out_down, 2, h, lo, n)
    tok_dev = places.shape[1]
    rows = groups * slot
    lanes = back_gate.shape[1]
    at = lax.broadcasted_iota(jnp.int32, (rows, tok_dev), 0)
    hit = (at == places[0:1, :]) | (at == places[1:2, :])
    grad_tokens[...] = lax.dot_general(
        jnp.where(hit, 1.0, 0.0).astype(bf), back_rows[...], FIRST,
        preferred_element_type=f32).astype(bf)
    sums = [jnp.zeros((1, tok_dev), f32), jnp.zeros((1, tok_dev), f32)]
    for j in range(groups):
        row = back_gate[j * SUM_ROWS:j * SUM_ROWS + 1, :]
        column = jnp.broadcast_to(row, (lanes, lanes)).T[0:slot, 0:1]
        here = lax.broadcasted_iota(jnp.int32, (slot, tok_dev), 0) + j * slot
        for k in range(2):
            sums[k] = sums[k] + jnp.sum(
                jnp.where(here == places[k:k + 1, :], column, 0.0), axis=0, keepdims=True)
    grad_gates[...] = jnp.concatenate(sums, axis=0) / weights[...].astype(f32)
    for copy in outs:
        copy.wait()


def on_device(tokens, cotangent, gate_weights, routes, w_gate, w_up, w_down):
    tok_dev, width = tokens.shape
    top_k = routes.shape[1]
    groups = lax.axis_size("ep")
    narrow = lax.axis_size("tp")
    capacity = 3 * top_k * tok_dev // (2 * groups)
    slot = -(-capacity // 16) * 16
    quarter = width // narrow
    ffe = w_gate.shape[2]
    rows = groups * slot
    lanes = -(-slot // 128) * 128
    stages = len(EIGHTHS) - 1
    span = max(b - a for a, b in zip(EIGHTHS, EIGHTHS[1:])) * groups // 8 * slot
    vmem = pl.BlockSpec(memory_space=pltpu.VMEM)
    hbm = pl.BlockSpec(memory_space=pl.ANY)
    bf, f32 = jnp.bfloat16, jnp.float32
    dma = pltpu.SemaphoreType.DMA
    per = dma((groups,))
    twice = dma((2, groups))
    routes_t = routes.T
    weights_t = gate_weights.T
    og, ou, od, back_rows, back_gate, places, hidden, c_rows = pl.pallas_call(
        functools.partial(expert_kernel, groups, slot, quarter),
        out_shape=(
            pltpu.VMEM((width, ffe), bf),
            pltpu.VMEM((width, ffe), bf),
            pltpu.VMEM((ffe, width), bf),
            pltpu.VMEM((rows, quarter), bf),
            pltpu.VMEM((groups * SUM_ROWS, lanes), f32),
            pltpu.VMEM((8, tok_dev), jnp.int32),
            pltpu.VMEM((rows, ffe), bf),
            pltpu.VMEM((rows, width), bf),
        ),
        in_specs=[vmem, vmem, hbm, hbm, hbm, hbm, hbm],
        out_specs=(vmem,) * 8,
        scratch_shapes=[
            pltpu.VMEM((tok_dev, width), bf),
            pltpu.VMEM((tok_dev, width), bf),
            pltpu.VMEM((rows, quarter), bf),
            pltpu.VMEM((rows, quarter), bf),
            pltpu.VMEM(((DIRECT[1] - DIRECT[0]) * slot, quarter), bf),
            pltpu.VMEM(((DIRECT[1] - DIRECT[0]) * slot, quarter), bf),
            pltpu.VMEM((rows, width), bf),
            pltpu.VMEM((width, ffe), bf),
            pltpu.VMEM((width, ffe), bf),
            pltpu.VMEM((ffe, width), bf),
            pltpu.VMEM((ffe, width), bf),
            pltpu.VMEM((ffe, width), bf),
            pltpu.VMEM((width, ffe), bf),
            pltpu.VMEM((span, ffe), f32),
            pltpu.VMEM((span, ffe), f32),
            pltpu.VMEM((span, ffe), f32),
            pltpu.VMEM((rows, 2 * ffe), bf),
            pltpu.VMEM((4, rows, quarter), bf),
            pltpu.VMEM((2, rows, quarter), bf),
            pltpu.VMEM((rows, quarter), bf),
            pltpu.VMEM((rows, quarter), bf),
            pltpu.VMEM((4, groups, lanes), f32),
            pltpu.VMEM((groups * SUM_ROWS, lanes), f32),
            dma((5,)),
            twice, twice, twice, twice, twice, twice, twice, twice,
            dma((2, stages)), dma((2, stages)),
            per, per, per, per,
            dma((3,)), dma((3,)),
            per, per,
            dma((3,)),
        ],
        compiler_params=pltpu.CompilerParams(
            collective_id=0, has_side_effects=True, vmem_limit_bytes=46 * 2 ** 20),
        name="expert",
    )(routes_t, weights_t, tokens, cotangent, w_gate[0], w_up[0], w_down[0])
    held = [pltpu.with_memory_space_constraint(x, pltpu.VMEM)
            for x in (places, back_rows, back_gate, hidden, c_rows, og, ou, od)]
    grad_tokens, grad_gates, grad_gate_w, grad_up_w, grad_down = pl.pallas_call(
        functools.partial(collect_kernel, groups, slot),
        out_shape=(
            jax.ShapeDtypeStruct((tok_dev, quarter), bf),
            jax.ShapeDtypeStruct((top_k, tok_dev), f32),
            jax.ShapeDtypeStruct((width, ffe), bf),
            jax.ShapeDtypeStruct((width, ffe), bf),
            jax.ShapeDtypeStruct((ffe, width), bf),
        ),
        in_specs=[vmem] * 9,
        out_specs=(vmem, vmem, hbm, hbm, hbm),
        scratch_shapes=[pltpu.VMEM((ffe, width), bf), dma((3, 4))],
        compiler_params=pltpu.CompilerParams(vmem_limit_bytes=12 * 2 ** 20),
        name="collect",
    )(held[0], weights_t, *held[1:])
    return (grad_tokens, grad_gates.T, grad_gate_w[None], grad_up_w[None], grad_down[None])


def solution(mesh):
    in_specs = (
        P("ep", None),
        P("ep", None),
        P("ep", None),
        P("ep", None),
        P("ep", None, "tp"),
        P("ep", None, "tp"),
        P("ep", "tp", None),
    )
    out_specs = (
        P("ep", "tp"),
        P("ep", None),
        P("ep", None, "tp"),
        P("ep", None, "tp"),
        P("ep", "tp", None),
    )
    return jax.shard_map(
        on_device, mesh=mesh, in_specs=in_specs, out_specs=out_specs, check_vma=False
    )
```
